32 devices in a mesh: ep: 8 (over z, y), tp: 4 (over x, core).
Axes of the slice: x: 2, y: 2, z: 4, core: 2. Of those that a mesh axis runs over, the one named last changes fastest.
Arguments:
- queries: bfloat16 [4096, 1024], P('ep', 'tp'), may hold values from -200 to 200
- keys: bfloat16 [4096, 256], P('ep', 'tp'), may hold values from -4 to 4
- values: bfloat16 [4096, 256], P('ep', 'tp'), may hold values from -4 to 4
- cum_gate: float32 [4096, 16], P(None, 'tp'), may hold values from -823 to 0, as said below
- out_weight: bfloat16 [1024, 2048], P('tp'), may hold values from -1.1953125 to 1.1953125
- moe_tokens: bfloat16 [4096, 2048], P(('ep', 'tp')), may hold values from -6 to 6
- norm_gain: float32 [2048], replicated, may hold values from 0.1 to 1.9
- routes: int32 [4096, 2], P('ep'), may hold values from 0 to 15, all different within a row; in each aligned block of 128 rows (0 to 127, 128 to 255, ...) at most 24 rows name the same one
- route_weight: float32 [4096, 2], P(('ep', 'tp')), may hold values from 0.25 to 2
- gate_weight: bfloat16 [16, 2048, 1024], P('ep', None, 'tp'), may hold values from -0.125 to 0.125
- up_weight: bfloat16 [16, 2048, 1024], P('ep', None, 'tp'), may hold values from -0.125 to 0.125
- down_weight: bfloat16 [16, 1024, 2048], P('ep', 'tp'), may hold values from -0.1875 to 0.1875
- shared_gate: bfloat16 [2048, 1024], P(None, 'tp'), may hold values from -0.125 to 0.125
- shared_up: bfloat16 [2048, 1024], P(None, 'tp'), may hold values from -0.125 to 0.125
- shared_down: bfloat16 [1024, 2048], P('tp'), may hold values from -0.1875 to 0.1875
Outputs:
- attn_out: bfloat16 [4096, 2048], P(('ep', 'tp'))
- moe_out: bfloat16 [4096, 2048], P(('ep', 'tp'))
The draws below stay inside these ranges and needn't reach their ends.
Inputs may be any that keep to these rules, and one draw needn't show every extreme that they name: `cum_gate`: each head's values never rise along positions. `routes`: each row names 2 different experts; among the rows of one device no expert is named by more than 24 rows, and some device reaches 24.
All inputs are finite; a program needn't handle non-finite values.
Results may differ from the reference program's by a relative error of at most 0.012.
Values may be sent and summed in bfloat16 or wider, within the bound.
A program may use at most 128 MiB of HBM per device.

```python
import math
import jax
import jax.numpy as jnp
import numpy as np
from jax import lax

D = 2048
QUERY_HEAD_COUNT = 16
KV_HEADS = 4
HEAD_SIZE = 64
FF = 1024
SHARED = 1024
TOPK = 2
QTOK_DEV = 512
MTOK_DEV = 128
SEQUENCE_LENGTH = 4096
MTOKENS = 4096
EXPERTS = 16
CAP = 24
N_TP = 4


def drawn_pair(key):
    base_offset = jax.random.fold_in(key, 11)
    key_query, key_keys = jax.random.split(base_offset, 2)
    key_array = jnp.clip(jax.random.normal(key_keys, (SEQUENCE_LENGTH, KV_HEADS * HEAD_SIZE), jnp.float32), -4.0, 4.0)
    query_array = jnp.clip(jax.random.normal(key_query, (SEQUENCE_LENGTH, QUERY_HEAD_COUNT * HEAD_SIZE), jnp.float32), -4.0, 4.0)
    return (query_array, key_array)


def draw_queries(key, part):
    return drawn_pair(key)[0].astype(jnp.bfloat16)


def draw_keys(key, part):
    return drawn_pair(key)[1].astype(jnp.bfloat16)


def draw_cum_gate(key, part):
    base_offset = jax.random.fold_in(key, 23)
    random_key_ordering, random_key_coarse, random_key_blocks, random_key_quick, random_key_gradual, random_key_spike, random_key_penalty = jax.random.split(base_offset, 7)
    fast_count = QUERY_HEAD_COUNT // 2
    is_fast = jax.random.permutation(random_key_ordering, QUERY_HEAD_COUNT) < fast_count
    roughness = jnp.exp(jax.random.uniform(random_key_coarse, (SEQUENCE_LENGTH, QUERY_HEAD_COUNT), jnp.float32, jnp.log(0.5), jnp.log(2.0)))
    block_count = SEQUENCE_LENGTH // QTOK_DEV
    factor = jnp.exp(jax.random.uniform(random_key_blocks, (block_count,), jnp.float32, jnp.log(0.4), jnp.log(2.5)))
    factor = jnp.repeat(factor, QTOK_DEV)[:, None]
    fast_rate = jax.random.uniform(random_key_quick, (QUERY_HEAD_COUNT,), jnp.float32, 1.0 / 50.0, 1.0 / 30.0)
    slow_rate = jnp.exp(jax.random.uniform(random_key_gradual, (QUERY_HEAD_COUNT,), jnp.float32, jnp.log(0.2), jnp.log(0.6))) / SEQUENCE_LENGTH
    head_rate = jnp.where(is_fast, fast_rate, slow_rate)
    step_logarithm = -head_rate[None, :] * roughness * factor
    spike_position = jax.random.randint(random_key_spike, (2,), 0, SEQUENCE_LENGTH)
    spike_loss_value = jax.random.uniform(random_key_penalty, (2, QUERY_HEAD_COUNT), jnp.float32, 0.2, 0.5)
    spike_hit_flag = (jnp.arange(SEQUENCE_LENGTH)[:, None] == spike_position[None, :]).astype(jnp.float32)
    step_logarithm = step_logarithm + jnp.dot(spike_hit_flag, jnp.log(1.0 - spike_loss_value))
    return jnp.cumsum(step_logarithm, axis=0)


def shard_levels(key, dims, cuts, low, top_value):
    loudness = 1.0
    for position, blocks in cuts:
        heights = jax.random.uniform(jax.random.fold_in(jax.random.fold_in(key, 6), position), (blocks,), jnp.float32, low / len(cuts), top_value / len(cuts))
        loudness = loudness * jnp.repeat(jnp.exp(heights), dims[position] // blocks).reshape((-1,) + (1,) * (len(dims) - 1 - position))
    return loudness


def assign_block(own_key, own, number, rows, number_of, top, most, slope):
    ranking = jax.random.permutation(own_key, number_of)
    heavy_load, usual = shares(number_of, rows * top, most, slope, True), shares(number_of, rows * top, most, slope, False)
    places = jnp.arange(number_of)

    def named(tallies, turn):
        used = int((tallies > 0).sum())
        fixed = max(1, used // 4)
        passed = fixed + (places - fixed + turn * (used - fixed)) % max(1, number_of - fixed)
        return jnp.zeros((number_of,), jnp.int32).at[ranking[jnp.where(places < fixed, places, passed)]].set(jnp.asarray(tallies, jnp.int32))

    tallies = jnp.where(number % 4 == 0, named(heavy_load, number // 4), named(usual, number - number // 4 - 1))
    mixed = jax.random.permutation(jax.random.fold_in(own, 3), number_of)
    giver, sink = mixed[0:number_of // 2 * 2:2], mixed[1:number_of // 2 * 2:2]
    margin = jnp.minimum(tallies[giver] - 1, most - tallies[sink]) // 2
    margin = jnp.where((giver == ranking[0]) | (sink == ranking[0]) | (tallies[sink] == 0), 0, jnp.maximum(margin, 0))
    passed = jax.random.randint(jax.random.fold_in(own, 4), (number_of // 2,), 0, 1 << 20) % (margin + 1)
    tallies = tallies.at[giver].add(-passed).at[sink].add(passed)
    labels = jnp.searchsorted(jnp.cumsum(tallies), jnp.arange(rows * top), side="right").astype(jnp.int32)
    listing = labels.reshape(top, rows).T
    listing = listing[jax.random.permutation(jax.random.fold_in(own, 1), rows)]
    turn = jax.random.randint(jax.random.fold_in(own, 2), (rows, 1), 0, top)
    return jnp.take_along_axis(listing, (jnp.arange(top)[None, :] + turn) % top, axis=1)


def shares(number_of, total, limit, slope, full):
    loads = [(1 << 20) // math.isqrt(standing ** slope) + 1 for standing in range(1, number_of + 1)]
    largest = limit if full else min(limit, max(-(-total // number_of), total * loads[0] // sum(loads)))
    least = 1 if total - largest >= number_of - 1 else 0
    holding, rest = [largest] + [least] * (number_of - 1), total - largest - least * (number_of - 1)
    while rest > 0:
        free = [i for i in range(1, number_of) if holding[i] < largest] or [i for i in range(1, number_of) if holding[i] < limit]
        pool, left = sum([loads[i] for i in free]), rest
        for i in free:
            more = min(limit - holding[i], max(1, left * loads[i] // pool), rest)
            holding[i] = holding[i] + more
            rest = rest - more
    return np.array(holding)


def gaussian(stream_key, extent, spread, most, shards=(), kind=jnp.bfloat16):
    values = jax.random.normal(stream_key, extent, jnp.float32) * spread
    if len(shards) > 0:
        values = shard_levels(stream_key, extent, shards, -0.22, 0.18) * values
    return jnp.clip(values, min=-most, max=most).astype(kind)


def setup_inputs(seed: int = 0) -> dict:
    seeds = jax.random.split(jax.random.key(seed), 16)
    queries = draw_queries(jax.random.fold_in(seeds[15], 71), 0)
    keys = draw_keys(jax.random.fold_in(seeds[15], 71), 0)
    values = gaussian(seeds[2], (SEQUENCE_LENGTH, KV_HEADS * HEAD_SIZE), 1.0, 4.0, ((0, 8), (1, 4)))
    cum_gate = draw_cum_gate(jax.random.fold_in(seeds[15], 71), 0)
    out_weight = gaussian(seeds[4], (QUERY_HEAD_COUNT * HEAD_SIZE, D), 0.2, 1.1953125, ((0, 4),))
    moe_tokens = gaussian(seeds[5], (MTOKENS, D), 1.0, 6.0, ((0, 32),))
    norm_gain = jnp.clip(1.0 + 0.18 * jax.random.normal(seeds[6], (D,), jnp.float32), 0.1, 1.9)
    routes_keys = jax.random.split(jax.random.fold_in(seeds[7], 1), MTOKENS // MTOK_DEV)
    routes_turns = jax.random.permutation(jax.random.fold_in(seeds[7], 3), MTOKENS // MTOK_DEV)
    routes = jax.vmap(lambda own, number: assign_block(jax.random.fold_in(seeds[7], 2), own, number, MTOK_DEV, EXPERTS, TOPK, CAP, 2))(routes_keys, routes_turns).reshape((MTOKENS, TOPK))
    route_weight = jnp.clip(jnp.exp(math.log(2.0) - 2.0794415 * jax.random.uniform(seeds[8], (MTOKENS, TOPK), jnp.float32) ** shard_levels(seeds[8], (MTOKENS, TOPK), ((0, 32),), -0.2, 0.2)), 0.25, 2.0)
    gate_weight = gaussian(seeds[9], (EXPERTS, D, FF), D ** -0.5, 0.125, ((0, 8), (2, 4)))
    up_weight = gaussian(seeds[10], (EXPERTS, D, FF), D ** -0.5, 0.125, ((0, 8), (2, 4)))
    down_weight = gaussian(seeds[11], (EXPERTS, FF, D), FF ** -0.5, 0.1875, ((0, 8), (1, 4)))
    shared_gate = gaussian(seeds[12], (D, SHARED), D ** -0.5, 0.125, ((1, 4),))
    shared_up = gaussian(seeds[13], (D, SHARED), D ** -0.5, 0.125, ((1, 4),))
    shared_down = gaussian(seeds[14], (SHARED, D), SHARED ** -0.5, 0.1875, ((0, 4),))
    return {"queries": queries, "keys": keys, "values": values, "cum_gate": cum_gate, "out_weight": out_weight, "moe_tokens": moe_tokens, "norm_gain": norm_gain, "routes": routes, "route_weight": route_weight, "gate_weight": gate_weight, "up_weight": up_weight, "down_weight": down_weight, "shared_gate": shared_gate, "shared_up": shared_up, "shared_down": shared_down}


def reference(queries, keys, values, cum_gate, out_weight, moe_tokens, norm_gain, routes, route_weight, gate_weight, up_weight, down_weight, shared_gate, shared_up, shared_down):
    group_size = QUERY_HEAD_COUNT // KV_HEADS
    block_len = math.gcd(SEQUENCE_LENGTH, 512)
    score_scale = HEAD_SIZE ** (-0.5)
    query_blocks = queries.reshape(SEQUENCE_LENGTH // block_len, block_len, QUERY_HEAD_COUNT, HEAD_SIZE)
    key_heads = keys.reshape(SEQUENCE_LENGTH, KV_HEADS, HEAD_SIZE).astype(jnp.float32)
    value_heads = values.reshape(SEQUENCE_LENGTH, KV_HEADS, HEAD_SIZE).astype(jnp.float32)
    gate_blocks = cum_gate.reshape(SEQUENCE_LENGTH // block_len, block_len, QUERY_HEAD_COUNT)
    key_gate = cum_gate.T.reshape(KV_HEADS, group_size, 1, SEQUENCE_LENGTH)
    key_pos = jnp.arange(SEQUENCE_LENGTH, dtype=jnp.int32)

    def attend(inputs):
        query_block, gate_block, number = inputs
        grouped = query_block.reshape(block_len, KV_HEADS, group_size, HEAD_SIZE).astype(jnp.float32)
        scores = jnp.einsum('tkgd,skd->kgts', grouped, key_heads) * score_scale
        scores = scores + gate_block.T.reshape(KV_HEADS, group_size, block_len, 1) - key_gate
        query_pos = number * block_len + jnp.arange(block_len, dtype=jnp.int32)
        causal = key_pos[None, :] <= query_pos[:, None]
        scores = jnp.where(causal, scores, -jnp.inf)
        weight = jnp.exp(scores - lax.optimization_barrier(jnp.max(scores, axis=-1, keepdims=True)))
        row_total = lax.optimization_barrier(jnp.sum(weight, axis=-1))
        rounded = lax.optimization_barrier(weight.astype(jnp.bfloat16)).astype(jnp.float32)
        mixed_heads = jnp.einsum('kgts,skd->kgtd', rounded, value_heads) / row_total[..., None]
        return mixed_heads.transpose(2, 0, 1, 3).reshape(block_len, QUERY_HEAD_COUNT * HEAD_SIZE).astype(jnp.bfloat16)
    mixed = lax.map(attend, (query_blocks, gate_blocks, jnp.arange(SEQUENCE_LENGTH // block_len, dtype=jnp.int32)))
    mixed = mixed.reshape(SEQUENCE_LENGTH, QUERY_HEAD_COUNT * HEAD_SIZE)
    head_width = QUERY_HEAD_COUNT * HEAD_SIZE // N_TP
    attn_sum = jnp.zeros((SEQUENCE_LENGTH, D), jnp.float32)
    for member in range(N_TP):
        partial_value = jnp.dot(mixed[:, member * head_width:(member + 1) * head_width], out_weight[member * head_width:(member + 1) * head_width], preferred_element_type=jnp.float32)
        attn_sum = attn_sum + partial_value.astype(jnp.bfloat16).astype(jnp.float32)
    attn_out = attn_sum.astype(jnp.bfloat16)
    token_f32 = moe_tokens.astype(jnp.float32)
    normed = (token_f32 * lax.rsqrt(lax.optimization_barrier(jnp.mean(token_f32 * token_f32, axis=-1, keepdims=True)) + 1e-06) * norm_gain.astype(jnp.float32)).astype(jnp.bfloat16)
    block_count = MTOKENS // MTOK_DEV
    flat_routes = routes.reshape(block_count, MTOK_DEV * TOPK)
    one_hot = (flat_routes[..., None] == jnp.arange(EXPERTS, dtype=jnp.int32)).astype(jnp.int32)
    slot_rank = lax.optimization_barrier(jnp.sum(one_hot * jnp.cumsum(one_hot, axis=1), axis=-1)) - 1
    slot_index = (jnp.arange(block_count, dtype=jnp.int32)[:, None] * CAP + slot_rank).reshape(-1)
    expert_flat = routes.reshape(-1)
    choice_row = jnp.arange(MTOKENS * TOPK, dtype=jnp.int32) // TOPK
    slot_total = block_count * CAP
    slot_token = jnp.full((EXPERTS, slot_total), MTOKENS, jnp.int32).at[expert_flat, slot_index].set(choice_row)
    slot_weight = jnp.zeros((EXPERTS, slot_total), jnp.float32).at[expert_flat, slot_index].set(route_weight.reshape(-1).astype(jnp.float32))
    padded = jnp.concatenate([normed, jnp.zeros((1, D), jnp.bfloat16)], axis=0)
    ff_width = FF // N_TP

    def apply_expert(summed, inputs):
        token_ids, weights_row, gate_one, up_one, down_one = inputs
        picked = padded[token_ids]
        hidden = (jax.nn.silu(jnp.dot(picked, gate_one, preferred_element_type=jnp.float32)) * jnp.dot(picked, up_one, preferred_element_type=jnp.float32)).astype(jnp.bfloat16)
        expert_sum = jnp.zeros((slot_total, D), jnp.float32)
        for member in range(N_TP):
            partial_value = jnp.dot(hidden[:, member * ff_width:(member + 1) * ff_width], down_one[member * ff_width:(member + 1) * ff_width], preferred_element_type=jnp.float32)
            expert_sum = expert_sum + partial_value.astype(jnp.bfloat16).astype(jnp.float32)
        expert_out = lax.optimization_barrier(expert_sum.astype(jnp.bfloat16)).astype(jnp.float32)
        return (summed.at[token_ids].add(weights_row[:, None] * expert_out), None)
    routed, _ = lax.scan(apply_expert, jnp.zeros((MTOKENS + 1, D), jnp.float32), (slot_token, slot_weight, gate_weight, up_weight, down_weight))
    shared_hidden = (jax.nn.silu(jnp.dot(normed, shared_gate, preferred_element_type=jnp.float32)) * jnp.dot(normed, shared_up, preferred_element_type=jnp.float32)).astype(jnp.bfloat16)
    shared_width = SHARED // N_TP
    shared_sum = jnp.zeros((MTOKENS, D), jnp.float32)
    for member in range(N_TP):
        partial_value = jnp.dot(shared_hidden[:, member * shared_width:(member + 1) * shared_width], shared_down[member * shared_width:(member + 1) * shared_width], preferred_element_type=jnp.float32)
        shared_sum = shared_sum + partial_value.astype(jnp.bfloat16).astype(jnp.float32)
    moe_out = (routed[:MTOKENS] + shared_sum).astype(jnp.bfloat16)
    return (attn_out, moe_out)
```

```python
import functools

import jax
import jax.numpy as jnp
from jax import lax
from jax.experimental import pallas as pl
from jax.experimental.pallas import tpu as pltpu
from jax.sharding import PartitionSpec as P

HEAD_SIZE = 64
EXP_DEV = 2
TOPK = 2


NEG_FILL = -1e30
EPSILON = 1e-06
LOG2E = 1.4426950408889634


def attend_kernel(heads, scale, block_ref, q_ref, kv_ref, bias_ref, out_ref, max_ref, acc_ref):
    rows = q_ref.shape[0]
    own = block_ref[0]
    max_ref[...] = jnp.full_like(max_ref, NEG_FILL)
    acc_ref[...] = jnp.zeros_like(acc_ref)

    def visit(block, diagonal):
        start = pl.multiple_of(block * rows, rows)
        keys = kv_ref[pl.ds(start, rows), :HEAD_SIZE]
        values = kv_ref[pl.ds(start, rows), HEAD_SIZE:]
        wide = jnp.concatenate([values, jnp.ones_like(values)], axis=1)
        for head in range(heads):
            query = q_ref[:, head * HEAD_SIZE : (head + 1) * HEAD_SIZE]
            scores = lax.dot_general(
                query, keys, (((1,), (1,)), ((), ())), preferred_element_type=jnp.float32
            )
            scores = scores * scale + bias_ref[head : head + 1, pl.ds(start, rows)]
            if diagonal:
                row_pos = lax.broadcasted_iota(jnp.int32, (rows, rows), 0)
                key_pos = lax.broadcasted_iota(jnp.int32, (rows, rows), 1)
                scores = jnp.where(key_pos <= row_pos, scores, NEG_FILL)
            old_max = max_ref[head, :, :1]
            new_max = jnp.maximum(old_max, jnp.max(scores, axis=1, keepdims=True))
            weight = jnp.exp2(scores - new_max).astype(jnp.bfloat16)
            part = jnp.dot(weight, wide, preferred_element_type=jnp.float32)
            acc_ref[head] = acc_ref[head] * jnp.exp2(old_max - new_max) + part
            max_ref[head] = jnp.broadcast_to(new_max, max_ref.shape[1:])

    def step(block, carry):
        visit(block, False)
        return carry

    visit(own, True)
    lax.fori_loop(0, own, step, 0)
    for head in range(heads):
        acc = acc_ref[head]
        out_ref[:, head * HEAD_SIZE : (head + 1) * HEAD_SIZE] = (
            acc[:, :HEAD_SIZE] / acc[:, HEAD_SIZE:]
        ).astype(out_ref.dtype)


def attention(queries, arrived_kv, cum_gate, ep_index):
    rows, width = queries.shape
    total = arrived_kv.shape[0]
    heads = width // HEAD_SIZE
    first = lax.dynamic_slice_in_dim(cum_gate, ep_index * rows, 1, 0)
    bias = ((first - cum_gate) * LOG2E).T
    return pl.pallas_call(
        functools.partial(attend_kernel, heads, HEAD_SIZE ** (-0.5) * LOG2E),
        out_shape=jax.ShapeDtypeStruct((rows, width), jnp.bfloat16),
        in_specs=[pl.BlockSpec(memory_space=pltpu.SMEM)]
        + [pl.BlockSpec(memory_space=pltpu.VMEM)] * 3,
        out_specs=pl.BlockSpec(memory_space=pltpu.VMEM),
        scratch_shapes=[
            pltpu.VMEM((heads, rows, 128), jnp.float32),
            pltpu.VMEM((heads, rows, 2 * HEAD_SIZE), jnp.float32),
        ],
        compiler_params=pltpu.CompilerParams(vmem_limit_bytes=32 * 1024 * 1024),
        cost_estimate=pl.CostEstimate(
            flops=4 * rows * total * width, bytes_accessed=total * 256, transcendentals=rows * total * heads
        ),
        name="attend",
    )(ep_index.reshape(1).astype(jnp.int32), queries, arrived_kv, bias)


def shards(
    queries,
    keys,
    values,
    cum_gate,
    out_weight,
    moe_tokens,
    norm_gain,
    routes,
    route_weight,
    gate_weight,
    up_weight,
    down_weight,
    shared_gate,
    shared_up,
    shared_down,
):
    ep_count = lax.axis_size("ep")
    tp_count = lax.axis_size("tp")
    ep_index = lax.axis_index("ep")
    tp_index = lax.axis_index("tp")
    arrived_kv = lax.all_gather(jnp.concatenate([keys, values], axis=1), "ep", axis=0, tiled=True)
    token_rows = moe_tokens.shape[0]
    model_width = moe_tokens.shape[1]
    token_f32 = moe_tokens.astype(jnp.float32)
    normed = (
        token_f32
        * lax.rsqrt(jnp.mean(token_f32 * token_f32, axis=-1, keepdims=True) + EPSILON)
        * norm_gain
    ).astype(jnp.bfloat16)
    experts_all = EXP_DEV * ep_count
    capacity = max(2, 3 * token_rows * TOPK // (2 * experts_all))
    slot_count = EXP_DEV * capacity
    per_device = routes.reshape(tp_count, token_rows * TOPK)
    one_hot = (per_device[..., None] == jnp.arange(experts_all, dtype=jnp.int32)).astype(jnp.int32)
    slot_rank = jnp.sum(one_hot * jnp.cumsum(one_hot, axis=1), axis=-1) - 1
    target = per_device // EXP_DEV
    local_expert = per_device % EXP_DEV
    own_target = lax.dynamic_index_in_dim(target, tp_index, 0, keepdims=False)
    own_local = lax.dynamic_index_in_dim(local_expert, tp_index, 0, keepdims=False)
    own_rank = lax.dynamic_index_in_dim(slot_rank, tp_index, 0, keepdims=False)
    own_place = own_target * slot_count + own_local * capacity + own_rank
    choice_row = jnp.arange(token_rows * TOPK, dtype=jnp.int32) // TOPK
    blank_row = jnp.zeros((1, model_width), jnp.bfloat16)
    source = jnp.full((ep_count * slot_count,), token_rows, jnp.int32).at[own_place].set(choice_row)
    padded = jnp.concatenate([normed, blank_row], axis=0)
    outgoing = padded[source].reshape(ep_count, slot_count, model_width)
    received = lax.all_to_all(outgoing, "ep", split_axis=0, concat_axis=0, tiled=True)
    received, arrived_kv = lax.optimization_barrier((received, arrived_kv))
    arrived = lax.all_gather(received, "tp", axis=1, tiled=True)
    mixed_heads = attention(queries, arrived_kv, cum_gate, ep_index)
    mixer_part = jnp.dot(mixed_heads, out_weight, preferred_element_type=jnp.float32).astype(
        jnp.bfloat16
    )
    arrived, mixer_part, normed_late = lax.optimization_barrier((arrived, mixer_part, normed))
    normed_group = lax.all_gather(normed_late, "tp", axis=0, tiled=True)
    expert_rows = arrived.reshape(ep_count * tp_count, EXP_DEV, capacity, model_width)
    gate_act = jnp.einsum(
        "secd,edf->secf", expert_rows, gate_weight, preferred_element_type=jnp.float32
    )
    up_act = jnp.einsum(
        "secd,edf->secf", expert_rows, up_weight, preferred_element_type=jnp.float32
    )
    hidden = (jax.nn.silu(gate_act) * up_act).astype(jnp.bfloat16)
    expert_part = jnp.einsum(
        "secf,efd->secd", hidden, down_weight, preferred_element_type=jnp.float32
    ).reshape(ep_count, tp_count * slot_count, model_width)
    expert_part, normed_group = lax.optimization_barrier(
        (expert_part.astype(jnp.bfloat16), normed_group)
    )
    expert_sum = lax.psum_scatter(expert_part, "tp", scatter_dimension=1, tiled=True)
    shared_hidden = (
        jax.nn.silu(jnp.dot(normed_group, shared_gate, preferred_element_type=jnp.float32))
        * jnp.dot(normed_group, shared_up, preferred_element_type=jnp.float32)
    ).astype(jnp.bfloat16)
    shared_part = jnp.dot(shared_hidden, shared_down, preferred_element_type=jnp.float32).astype(
        jnp.bfloat16
    )
    both_part = jnp.concatenate([mixer_part, shared_part], axis=1)
    expert_sum, both_part = lax.optimization_barrier((expert_sum, both_part))
    both_sum = lax.psum_scatter(both_part, "tp", scatter_dimension=0, tiled=True)
    mixer_sum = both_sum[:, :model_width]
    shared_sum = both_sum[:, model_width:].astype(jnp.float32)
    returned = lax.all_to_all(expert_sum, "ep", split_axis=0, concat_axis=0, tiled=True)
    picked = returned.reshape(ep_count * slot_count, model_width)[own_place].reshape(
        token_rows, TOPK, model_width
    )
    routed = jnp.sum(route_weight[..., None] * picked.astype(jnp.float32), axis=1)
    moe_out = (routed + shared_sum).astype(jnp.bfloat16)
    return (mixer_sum, moe_out)


def solution(mesh):
    in_specs = (
        P("ep", "tp"),
        P("ep", "tp"),
        P("ep", "tp"),
        P(None, "tp"),
        P("tp", None),
        P(("ep", "tp"), None),
        P(),
        P("ep", None),
        P(("ep", "tp"), None),
        P("ep", None, "tp"),
        P("ep", None, "tp"),
        P("ep", "tp", None),
        P(None, "tp"),
        P(None, "tp"),
        P("tp", None),
    )
    out_specs = (P(("ep", "tp"), None), P(("ep", "tp"), None))
    return jax.shard_map(shards, mesh=mesh, in_specs=in_specs, out_specs=out_specs, check_vma=False)
```
